32 devices in a mesh: sp: 16 (over z, y, x), tp: 2 (over core).
Axes of the slice: x: 2, y: 2, z: 4, core: 2. Of those that a mesh axis runs over, the one named last changes fastest.
Arguments:
- queries: bfloat16 [8192, 2048], P('sp', 'tp'), may hold values from -6 to 6
- keys: bfloat16 [8192, 1024], P('sp', 'tp'), may hold values from -6 to 6
- values: bfloat16 [8192, 1024], P('sp', 'tp'), may hold values from -6 to 6
- documents: int32 [8192], P('sp'), may hold values from 0 to 3, never falling along the last dimension, each value on 1 to 4096 neighbouring positions
- query_gain: float32 [128], replicated, may hold values from 1.8 to 6
- key_gain: float32 [128], replicated, may hold values from 1.8 to 6
- residual: bfloat16 [8192, 4096], P('sp', 'tp'), may hold values from -6 to 6
- out_weight: bfloat16 [2048, 4096], P('tp'), may hold values from -0.125 to 0.125
- norm_gain: float32 [4096], replicated, may hold values from 0.1 to 1.9
- up_weight: bfloat16 [4096, 16384], P('sp', 'tp'), may hold values from -0.09375 to 0.09375
- down_weight: bfloat16 [16384, 4096], P('tp', 'sp'), may hold values from -0.046875 to 0.046875
Outputs:
- mixed: bfloat16 [8192, 4096], P('sp', 'tp')
The draws below stay inside these ranges and needn't reach their ends.
Inputs may be any that keep to these rules, and one draw needn't show every extreme that they name: `documents`: document numbers never fall along the sequence; a document has at most 4096 positions.
All inputs are finite; a program needn't handle non-finite values.
Results may differ from the reference program's by a relative error of at most 0.017.
The reference program's roundings to bfloat16 on the way count: a program that leaves them out, or rounds other values in their place, can miss the bound.
Values may be sent and summed in bfloat16 or wider, within the bound.
A program may use at most 256 MiB of HBM per device.

```python
import math
import jax
import jax.numpy as jnp
import numpy as np
from jax import lax

D = 4096
FF = 16384
HQ = 16
KV = 8
HD = 128
GRID_W = 64
TOK_DEV = 512
TOKENS = 8192
DOCS = 4
DOC_MOST = 4096
N_SP = 16
N_TP = 2


def drawn_keys(key):
    base = jnp.clip(jax.random.normal(jax.random.fold_in(key, 11), (TOKENS, KV * HD), jnp.float32), -6.0, 6.0)
    return base


def draw_keys(key, part):
    return drawn_keys(key).astype(jnp.bfloat16)


def draw_queries(key, part):
    base = jnp.clip(jax.random.normal(jax.random.fold_in(key, 12), (TOKENS, HQ * HD), jnp.float32), -6.0, 6.0)
    return base.astype(jnp.bfloat16)


def gain_values(key, offset):
    return jax.random.uniform(jax.random.fold_in(key, offset), (HD,), jnp.float32, 1.8, 3.0)


def draw_query_gain(key, part):
    return gain_values(key, 21)


def draw_key_gain(key, part):
    return gain_values(key, 22)


def steps_of(rng, dims, cuts, smallest, top_value):
    def one(axis_at, blocks):
        steps = jax.random.uniform(jax.random.fold_in(jax.random.fold_in(rng, 6), axis_at), (blocks,), jnp.float32, smallest / len(cuts), top_value / len(cuts))
        return jnp.repeat(jnp.exp(steps), dims[axis_at] // blocks).reshape((-1,) + (1,) * (len(dims) - axis_at - 1))

    level = one(*cuts[0])
    for cut in cuts[1:]:
        level = level * one(*cut)
    return level


def split_up(count, total, bound, skew):
    loads = [(1 << 20) // math.isqrt(rank ** skew) + 1 for rank in range(2, count + 1)]
    rest, counts = total - bound - (count - 1), [1] * (count - 1)
    while rest > 0:
        movable = [i for i in range(count - 1) if counts[i] < bound]
        pool, remaining = sum([loads[i] for i in movable]), rest
        for i in movable:
            extra = min(bound - counts[i], max(1, remaining * loads[i] // pool), rest)
            counts[i] = counts[i] + extra
            rest = rest - extra
    return np.array([bound] + counts)


def ragged_sizes(own_key, amount, total, bound, slope):
    if amount == 2:
        one = jax.random.randint(own_key, (), max(1, total - bound), min(bound, total - 1) + 1)
        return jnp.stack([one, total - one])
    sizes = jnp.asarray(split_up(amount, total, bound, slope), jnp.int32)
    couples = (amount - 1) // 2
    giver, receiver = sizes[1:1 + 2 * couples:2], sizes[2:2 + 2 * couples:2]
    margin = jnp.minimum(giver - 1, bound - receiver)
    passed = jax.random.randint(jax.random.fold_in(own_key, 1), (couples,), 0, 1 << 20) % (margin + 1)
    sizes = sizes.at[1:1 + 2 * couples:2].set(giver - passed).at[2:2 + 2 * couples:2].set(receiver + passed)
    return sizes[jax.random.permutation(jax.random.fold_in(own_key, 2), amount)]


def scatter_about(own_key, shape, spread, bound, split=(), kind=jnp.bfloat16):
    level = steps_of(own_key, shape, split, -0.22, 0.18) if split else 1.0
    values = jax.random.normal(own_key, shape, jnp.float32) * spread * level
    return jnp.minimum(jnp.maximum(values, -bound), bound).astype(kind)


def setup_inputs(seed: int = 0) -> dict:
    seeds = jax.random.split(jax.random.key(seed), 12)
    return {
        "queries": draw_queries(jax.random.fold_in(seeds[11], 71), 0),
        "keys": draw_keys(jax.random.fold_in(seeds[11], 71), 0),
        "values": scatter_about(seeds[2], (TOKENS, KV * HD), 1.0, 6.0, ((0, 16), (1, 2))),
        "documents": jnp.searchsorted(jnp.cumsum(ragged_sizes(seeds[3], DOCS, TOKENS, DOC_MOST, 0)), jnp.arange(TOKENS), side="right").astype(jnp.int32),
        "query_gain": draw_query_gain(jax.random.fold_in(seeds[11], 71), 0),
        "key_gain": draw_key_gain(jax.random.fold_in(seeds[11], 71), 0),
        "residual": scatter_about(seeds[6], (TOKENS, D), 1.0, 6.0, ((0, 16), (1, 2))),
        "out_weight": scatter_about(seeds[7], (HQ * HD, D), (HQ * HD) ** -0.5, 0.125, ((0, 2),)),
        "norm_gain": jnp.clip(1.0 + 0.18 * jax.random.normal(seeds[8], (D,), jnp.float32), 0.1, 1.9),
        "up_weight": scatter_about(seeds[9], (D, FF), D ** -0.5, 0.09375, ((0, 16), (1, 2))),
        "down_weight": scatter_about(seeds[10], (FF, D), FF ** -0.5, 0.046875, ((0, 2), (1, 16))),
    }


norm_eps = 1e-06
rope_base = 10000.0
masked_score = -1e+30

def head_norm(heads_in, gain):
    values32 = heads_in.astype(jnp.float32)
    scaled = values32 * lax.rsqrt(lax.optimization_barrier(jnp.mean(values32 * values32, axis=-1, keepdims=True)) + norm_eps)
    return scaled * gain.astype(jnp.float32)

def rotate_half(heads_in, position):
    quarter = heads_in.shape[-1] // 2
    inverse_freq = rope_base ** (-jnp.arange(quarter, dtype=jnp.float32) / quarter)
    angles = position[:, None] * inverse_freq[None, :]
    cosine_part = jnp.cos(angles)[:, None, :]
    sine_part = jnp.sin(angles)[:, None, :]
    leading = heads_in[..., :quarter]
    trailing = heads_in[..., quarter:]
    return jnp.concatenate([leading * cosine_part - trailing * sine_part, leading * sine_part + trailing * cosine_part], axis=-1)

def grid_rotary(heads_in, positions):
    half_width = heads_in.shape[-1] // 2
    grid_row = (positions // GRID_W).astype(jnp.float32)
    grid_col = (positions % GRID_W).astype(jnp.float32)
    return jnp.concatenate([rotate_half(heads_in[..., :half_width], grid_row), rotate_half(heads_in[..., half_width:], grid_col)], axis=-1)

def reference(queries, keys, values, documents, query_gain, key_gain, residual, out_weight, norm_gain, up_weight, down_weight):
    group_size = HQ // KV
    positions = jnp.arange(TOKENS, dtype=jnp.int32)
    queries_rot = grid_rotary(head_norm(queries.reshape(TOKENS, HQ, HD), query_gain), positions).astype(jnp.bfloat16)
    keys_rot = grid_rotary(head_norm(keys.reshape(TOKENS, KV, HD), key_gain), positions).astype(jnp.bfloat16)
    key_float = keys_rot.astype(jnp.float32)
    value_float = values.reshape(TOKENS, KV, HD).astype(jnp.float32)
    query_blocks = queries_rot.reshape(N_SP, TOK_DEV, KV, group_size, HD)
    doc_blocks = documents.reshape(N_SP, TOK_DEV)

    def attend(block_pair):
        query_block, doc_block = block_pair
        scores = jnp.einsum('qkgd,skd->kgqs', query_block.astype(jnp.float32), key_float) * HD ** (-0.5)
        same_doc = doc_block[:, None] == documents[None, :]
        scores = jnp.where(same_doc, scores, masked_score)
        row_max = lax.optimization_barrier(jnp.max(scores, axis=-1, keepdims=True))
        probs = jnp.where(same_doc, jnp.exp(scores - row_max), 0.0)
        row_sum = lax.optimization_barrier(jnp.sum(probs, axis=-1))
        probs_low = lax.optimization_barrier(probs.astype(jnp.bfloat16)).astype(jnp.float32)
        summed = jnp.einsum('kgqs,skd->qkgd', probs_low, value_float)
        return (summed / jnp.transpose(row_sum, (2, 0, 1))[..., None]).astype(jnp.bfloat16)
    attended = lax.map(attend, (query_blocks, doc_blocks)).reshape(TOKENS, HQ * HD)
    head_width = HQ * HD // N_TP
    branch = jnp.zeros((TOKENS, D), jnp.float32)
    for head_block in range(N_TP):
        lower = head_block * head_width
        part_sum = jnp.dot(attended[:, lower:lower + head_width], out_weight[lower:lower + head_width], preferred_element_type=jnp.float32)
        branch = branch + lax.optimization_barrier(part_sum.astype(jnp.bfloat16)).astype(jnp.float32)
    stream = residual.astype(jnp.float32) + branch
    normed = stream * lax.rsqrt(lax.optimization_barrier(jnp.mean(stream * stream, axis=-1, keepdims=True)) + norm_eps)
    normed = (normed * norm_gain.astype(jnp.float32)).astype(jnp.bfloat16)
    hidden = jnp.dot(normed, up_weight, preferred_element_type=jnp.float32)
    positive = jnp.maximum(hidden, 0.0)
    squared = (positive * positive).astype(jnp.bfloat16)
    unit_width = FF // N_TP
    feed = jnp.zeros((TOKENS, D), jnp.float32)
    for unit_block in range(N_TP):
        lower = unit_block * unit_width
        part_sum = jnp.dot(squared[:, lower:lower + unit_width], down_weight[lower:lower + unit_width], preferred_element_type=jnp.float32)
        feed = feed + lax.optimization_barrier(part_sum.astype(jnp.bfloat16)).astype(jnp.float32)
    return (stream + feed).astype(jnp.bfloat16)
```

```python
import functools

import jax
import jax.numpy as jnp
from jax import lax
from jax.experimental import pallas as pl
from jax.experimental.layout import Layout, with_layout_constraint
from jax.experimental.pallas import tpu as pltpu
from jax.sharding import PartitionSpec as P


HQ = 16
KV = 8
HD = 128
GRID_W = 64


norm_eps = 1e-06
rope_base = 10000.0
masked_score = -1e30
log2e = 1.4426950408889634


def head_norm(heads_in, gain):
    values32 = heads_in.astype(jnp.float32)
    scaled = values32 * lax.rsqrt(jnp.mean(values32 * values32, axis=-1, keepdims=True) + norm_eps)
    return scaled * gain


def rotate_half(heads_in, position):
    quarter = heads_in.shape[-1] // 2
    inverse_freq = rope_base ** (-jnp.arange(quarter, dtype=jnp.float32) / quarter)
    angles = position[:, None] * inverse_freq[None, :]
    cosine_part = jnp.cos(angles)[:, None, :]
    sine_part = jnp.sin(angles)[:, None, :]
    leading = heads_in[..., :quarter]
    trailing = heads_in[..., quarter:]
    return jnp.concatenate(
        [
            leading * cosine_part - trailing * sine_part,
            leading * sine_part + trailing * cosine_part,
        ],
        axis=-1,
    )


def grid_rotary(heads_in, positions):
    half_width = heads_in.shape[-1] // 2
    grid_row = (positions // GRID_W).astype(jnp.float32)
    grid_col = (positions % GRID_W).astype(jnp.float32)
    return jnp.concatenate(
        [
            rotate_half(heads_in[..., :half_width], grid_row),
            rotate_half(heads_in[..., half_width:], grid_col),
        ],
        axis=-1,
    )


def row_major(array):
    return with_layout_constraint(array, Layout(major_to_minor=(0, 1)))


def from_behind(array, shift, size):
    return lax.ppermute(array, "tp", [(i, (i + shift) % size) for i in range(size)])


def gather_body(
    queries,
    keys,
    values,
    documents,
    query_gain,
    key_gain,
    residual,
    out_weight,
    norm_gain,
    up_weight,
    down_weight,
):
    tok_rows = queries.shape[0]
    key_heads = keys.shape[1] // HD
    group_size = HQ // KV
    width_local = residual.shape[1]
    tp_index = lax.axis_index("tp")
    up_whole = lax.all_gather(up_weight, "sp", axis=0, tiled=True)
    tp_size = lax.axis_size("tp")
    residual_whole = jnp.zeros((tok_rows, width_local * tp_size), jnp.bfloat16)
    residual_whole = lax.dynamic_update_slice_in_dim(
        residual_whole, residual, tp_index * width_local, 1
    )
    for shift in range(1, tp_size):
        owner = (tp_index - shift) % tp_size
        residual_whole = lax.dynamic_update_slice_in_dim(
            residual_whole, from_behind(residual, shift, tp_size), owner * width_local, 1
        )
    positions = lax.axis_index("sp") * tok_rows + jnp.arange(tok_rows, dtype=jnp.int32)
    queries_rot = grid_rotary(
        head_norm(queries.reshape(tok_rows, key_heads * group_size, HD), query_gain), positions
    )
    queries_rot = queries_rot.astype(jnp.bfloat16).reshape(tok_rows, key_heads, group_size, HD)
    keys_rot = grid_rotary(
        head_norm(keys.reshape(tok_rows, key_heads, HD), key_gain), positions
    ).astype(jnp.bfloat16)
    value_heads = values.reshape(tok_rows, key_heads, HD)
    own_docs = documents.astype(jnp.bfloat16)
    score_scale = HD ** (-0.5)
    key_value = jnp.concatenate(
        [keys_rot.reshape(tok_rows, key_heads * HD), value_heads.reshape(tok_rows, key_heads * HD)],
        axis=1,
    )
    key_value = lax.all_gather(key_value, "sp", axis=0, tiled=True)
    doc_piece = lax.all_gather(own_docs, "sp", axis=0, tiled=True)
    same_doc = own_docs[:, None] == doc_piece[None, :]
    head_queries = queries_rot.reshape(tok_rows, key_heads * group_size, HD).swapaxes(0, 1)

    def attend(query_head):
        head, query = query_head
        key_at = head // group_size * HD
        key_piece = lax.dynamic_slice_in_dim(key_value, key_at, HD, 1)
        value_piece = lax.dynamic_slice_in_dim(key_value, key_at + key_heads * HD, HD, 1)
        scores = jnp.einsum("qd,sd->qs", query, key_piece, preferred_element_type=jnp.float32)
        scores = jnp.where(same_doc, scores * score_scale, masked_score)
        row_max = jnp.max(scores, axis=-1, keepdims=True)
        probs = jnp.where(same_doc, jnp.exp(scores - row_max), 0.0)
        row_sum = jnp.sum(probs, axis=-1)
        update = jnp.dot(
            probs.astype(jnp.bfloat16), value_piece, preferred_element_type=jnp.float32
        )
        return (update / row_sum[:, None]).astype(jnp.bfloat16)

    attended = lax.map(attend, (jnp.arange(key_heads * group_size), head_queries))
    down_late, attended = lax.optimization_barrier((row_major(down_weight.T), attended))
    down_whole = lax.all_gather(down_late, "sp", axis=0, tiled=True)
    attended = attended.swapaxes(0, 1)
    attended = attended.reshape(tok_rows, key_heads * group_size * HD)
    partial_out = jnp.dot(attended, out_weight, preferred_element_type=jnp.float32)
    partial_out = partial_out.astype(jnp.bfloat16)
    branch = partial_out.astype(jnp.float32)
    for shift in range(1, tp_size):
        branch = branch + from_behind(partial_out, shift, tp_size).astype(jnp.float32)
    stream_whole = residual_whole.astype(jnp.float32) + branch
    normed = stream_whole * lax.rsqrt(
        jnp.mean(stream_whole * stream_whole, axis=-1, keepdims=True) + norm_eps
    )
    normed = (normed * norm_gain).astype(jnp.bfloat16)
    stream = lax.dynamic_slice_in_dim(stream_whole, tp_index * width_local, width_local, 1)
    hidden = jnp.dot(normed, up_whole, preferred_element_type=jnp.float32)
    positive = jnp.maximum(hidden, 0.0)
    squared = (positive * positive).astype(jnp.bfloat16)
    product = lax.dot_general(
        squared, down_whole, (((1,), (1,)), ((), ())), preferred_element_type=jnp.float32
    )
    product = product.astype(jnp.bfloat16)
    feed = lax.dynamic_slice_in_dim(product, tp_index * width_local, width_local, 1)
    feed = feed.astype(jnp.float32)
    for shift in range(1, tp_size):
        target = (tp_index + shift) % tp_size
        piece = lax.dynamic_slice_in_dim(product, target * width_local, width_local, 1)
        feed = feed + from_behind(piece, shift, tp_size).astype(jnp.float32)
    return (stream + feed).astype(jnp.bfloat16)


def prepare_kernel(heads, group, q_ref, k_ref, v_ref, cos_ref, sin_ref, qg_ref, kg_ref, o_ref):
    cosine = cos_ref[...]
    sine = sin_ref[...]
    lane = lax.broadcasted_iota(jnp.int32, cosine.shape, 1)
    first = (lane % (HD // 2)) < HD // 4

    def turned(u, gain):
        u = u.astype(jnp.float32)
        u = u * lax.rsqrt(jnp.mean(u * u, axis=-1, keepdims=True) + norm_eps) * gain
        ahead = pltpu.roll(u, HD - HD // 4, 1)
        behind = pltpu.roll(u, HD // 4, 1)
        return (u * cosine + jnp.where(first, ahead, behind) * sine).astype(jnp.bfloat16)

    q_gain = qg_ref[...]
    k_gain = kg_ref[...]
    for h in range(heads):
        for g in range(group):
            at = (h * group + g) * HD
            o_ref[h, :, g * HD : (g + 1) * HD] = turned(q_ref[:, at : at + HD], q_gain)
        at = h * HD
        o_ref[h, :, group * HD : (group + 1) * HD] = turned(k_ref[:, at : at + HD], k_gain)
        o_ref[h, :, (group + 1) * HD :] = v_ref[:, at : at + HD]


def prepare(queries, keys, values, positions, query_gain, key_gain):
    rows = queries.shape[0]
    heads = keys.shape[1] // HD
    group = HQ // KV
    lane = jnp.arange(HD, dtype=jnp.int32)
    quarter = HD // 4
    freq = rope_base ** (-(lane % quarter).astype(jnp.float32) / quarter)
    grid_row = (positions // GRID_W).astype(jnp.float32)
    grid_col = (positions % GRID_W).astype(jnp.float32)
    where_at = jnp.where(lane[None, :] < HD // 2, grid_row[:, None], grid_col[:, None])
    angles = where_at * freq[None, :]
    cosine = jnp.cos(angles)
    sine = jnp.where((lane % (HD // 2)) < quarter, -1.0, 1.0)[None, :] * jnp.sin(angles)
    block = min(rows, 128)
    width = (group + 2) * HD
    row_block = lambda cols: pl.BlockSpec((block, cols), lambda i: (i, 0))
    fixed = pl.BlockSpec((1, HD), lambda i: (0, 0))
    return pl.pallas_call(
        functools.partial(prepare_kernel, heads, group),
        grid=(rows // block,),
        out_shape=jax.ShapeDtypeStruct((heads, rows, width), jnp.bfloat16),
        in_specs=[
            row_block(heads * group * HD),
            row_block(heads * HD),
            row_block(heads * HD),
            row_block(HD),
            row_block(HD),
            fixed,
            fixed,
        ],
        out_specs=pl.BlockSpec((heads, block, width), lambda i: (0, i, 0)),
        cost_estimate=pl.CostEstimate(flops=rows * 20000, bytes_accessed=rows * 8192, transcendentals=0),
        name="prepare",
    )(queries, keys, values, cosine, sine, query_gain.reshape(1, HD), key_gain.reshape(1, HD))


def attend_kernel(group, key_block, slots, span_ref, q_ref, kv_ref, qdoc_ref, kdoc_ref, o_ref):
    tile = pl.program_id(0)
    lo = span_ref[0, tile]
    hi = span_ref[1, tile]
    plane = span_ref[4, tile]
    rows = q_ref.shape[0]
    per_slot = kv_ref.shape[0] // slots
    query = jnp.concatenate([q_ref[:, g * HD : (g + 1) * HD] for g in range(group)], axis=0)
    q_doc = jnp.concatenate([qdoc_ref[...]] * group, axis=0)
    factor = HD ** (-0.5) * log2e

    def step(block, carry):
        top, total, out = carry
        slot = lax.rem(plane + slots - block // per_slot, slots)
        at = slot * per_slot + lax.rem(block, per_slot)
        key = kv_ref[at, :key_block, :HD]
        value = kv_ref[at, :key_block, HD:]
        scores = lax.dot_general(
            query, key, (((1,), (1,)), ((), ())), preferred_element_type=jnp.float32
        )
        k_doc = kdoc_ref[block]
        scores = jnp.where(q_doc == k_doc, scores, masked_score)
        new_top = jnp.maximum(top, jnp.max(scores, axis=-1, keepdims=True))
        probs = jnp.exp2((scores - new_top) * factor)
        fade = jnp.exp2((top - new_top) * factor)
        total = total * fade + jnp.sum(probs, axis=-1, keepdims=True)
        out = out * fade + jnp.dot(
            probs.astype(jnp.bfloat16), value, preferred_element_type=jnp.float32
        )
        return new_top, total, out

    start = (
        jnp.full((group * rows, 1), masked_score, jnp.float32),
        jnp.zeros((group * rows, 1), jnp.float32),
        jnp.zeros((group * rows, HD), jnp.float32),
    )
    _, total, out = lax.fori_loop(lo, hi, step, start)
    out = (out / total).astype(jnp.bfloat16)
    for g in range(group):
        o_ref[:, g * HD : (g + 1) * HD] = out[g * rows : (g + 1) * rows]


doc_pad = 16


def attention(packed, key_value, docs, plane, group, slots):
    rows = packed.shape[0]
    tile = min(256, rows)
    key_block = key_value.shape[1] - doc_pad
    own = lax.dynamic_slice_in_dim(docs, plane * rows, rows)
    q_low = own[::tile]
    q_high = own[tile - 1 :: tile]
    k_low = docs[::key_block]
    k_high = docs[key_block - 1 :: key_block]
    lo = jnp.sum(k_high[None, :] < q_low[:, None], axis=1).astype(jnp.int32)
    hi = jnp.sum(k_low[None, :] <= q_high[:, None], axis=1).astype(jnp.int32)
    span = jnp.stack([lo, hi, q_low, q_high, jnp.full_like(lo, plane)])
    blocks = docs.shape[0] // key_block
    grid_spec = pltpu.PrefetchScalarGridSpec(
        num_scalar_prefetch=1,
        grid=(rows // tile,),
        in_specs=[
            pl.BlockSpec((tile, group * HD), lambda i, s: (i, 0)),
            pl.BlockSpec(key_value.shape, lambda i, s: (0, 0, 0)),
            pl.BlockSpec((tile, 1), lambda i, s: (i, 0)),
            pl.BlockSpec((blocks, 1, key_block), lambda i, s: (0, 0, 0)),
        ],
        out_specs=pl.BlockSpec((tile, group * HD), lambda i, s: (i, 0)),
    )
    work = group * rows * docs.shape[0] // 2
    return pl.pallas_call(
        functools.partial(attend_kernel, group, key_block, slots),
        grid_spec=grid_spec,
        out_shape=jax.ShapeDtypeStruct((rows, group * HD), jnp.bfloat16),
        compiler_params=pltpu.CompilerParams(vmem_limit_bytes=48 * 1024 * 1024),
        cost_estimate=pl.CostEstimate(
            flops=work * 4 * HD, bytes_accessed=key_value.size * 2, transcendentals=work
        ),
        name="attention",
    )(span, packed, key_value, own.reshape(rows, 1), docs.reshape(blocks, 1, key_block))


MESH = pl.DeviceIdType.MESH


def feed_kernel(
    outer, inner, tok, width, units,
    normed_ref, up_own, up_odd, down_own, late_u2, late_d2, late_d3, late_d1,
    own_ref, ends_ref, mids_ref, last_ref, tok_a, tok_b, given_s, given_r, send_e, send_x, send_l, land_u, land_d,
    up_v, down_v, tok_v, sq_v, stage_v, recv_v, add_v, sum_v,
    way_s, way_r, pair_s, pair_r, give_s, give_r, e_s, e_r, x_s, x_r, l_s, l_r, w_s, w_r, loc, big,
):
    me = lax.axis_index("sp")
    core = lax.axis_index("tp")
    z = me // inner
    i = me % inner
    mid = ((z + 1) // 2) % 2
    near = (z + 1 - 2 * (z % 2)) * inner + i
    across = (outer - 1 - z) * inner + i
    half = tok // 2

    barrier = pltpu.get_barrier_semaphore()
    beside = [{"sp": z * inner + i + bit - 2 * bit * ((i // bit) % 2)} for bit in (1, 2)]
    for peer in ({"sp": near}, {"sp": across}, {"tp": 1 - core}, *beside):
        pl.semaphore_signal(barrier, inc=1, device_id=peer, device_id_type=MESH)
    pl.semaphore_wait(barrier, 5)

    def remote(src, dst, send, recv, peer):
        return pltpu.make_async_remote_copy(
            src_ref=src, dst_ref=dst, send_sem=send, recv_sem=recv, device_id=peer, device_id_type=MESH
        )

    def local(src, dst, sem):
        copy = pltpu.make_async_copy(src, dst, sem)
        copy.start()
        copy.wait()

    to_near, to_across, to_core = {"sp": near}, {"sp": across}, {"tp": 1 - core}
    own_near = remote(normed_ref, tok_a.at[1], way_s.at[0], way_r.at[1], to_near)
    own_across = remote(normed_ref, tok_a.at[3], way_s.at[1], way_r.at[3], to_across)
    near_across = remote(tok_a.at[1], tok_a.at[2], way_s.at[2], way_r.at[2], to_across)
    across_near = remote(tok_a.at[3], tok_a.at[2], way_s.at[3], way_r.at[2], to_near)
    far_near = remote(tok_a.at[2], tok_a.at[3], way_s.at[4], way_r.at[3], to_near)

    def token_pair(q):
        src = normed_ref if isinstance(q, int) and q == 0 else tok_a.at[q]
        return remote(src, tok_b.at[q], pair_s.at[q], pair_r.at[q], to_core)

    def arrived(q):
        remote(tok_a.at[q], tok_a.at[q], way_s.at[0], way_r.at[q], to_near).wait_recv()
        token_pair(q).start()

    own_near.start()
    token_pair(0).start()
    depth = late_u2.shape[0]
    plane_of = (z, z + 1 - 2 * (z % 2), (z + 2) % 4, 3 - z)
    peers = {bit: {"sp": z * inner + i + bit - 2 * bit * ((i // bit) % 2)} for bit in (1, 2)}
    items = [
        (late_u2, land_u, 2, (1, 2)),
        (late_d2, land_d.at[0], 2, (2, 1)),
        (late_d3, land_d.at[1], 3, (1, 2)),
        (late_d1, land_d.at[2], 1, (2, 1)),
    ]

    def leg(n, j):
        src, land, _, (first, second) = items[n]
        from_ref = src if j < 3 else land.at[first - 1]
        return remote(
            from_ref, land.at[j - 1], w_s.at[n, j - 1], w_r.at[n, j - 1], peers[second if j == 3 else j]
        )

    def send_item(n):
        first, second = items[n][3]
        leg(n, first).start()
        leg(n, second).start()

    def forward_item(n):
        leg(n, items[n][3][0]).wait_recv()
        leg(n, 3).start()

    def into(weights, plane, j, src, sem):
        at = pl.ds(pl.multiple_of((plane * inner + j) * depth, depth), depth)
        dst = up_v.at[at] if weights == 0 else down_v.at[:, at]
        return pltpu.make_async_copy(src, dst, sem)

    loads = [], []
    for j in range(inner):
        loads[0].append(into(0, plane_of[0], j, up_own.at[j], big.at[0, 0, j]))
        for n, k in enumerate((1, 3)):
            src = up_odd.at[j, n * depth : (n + 1) * depth]
            loads[0].append(into(0, plane_of[k], j, src, big.at[0, k, j]))
        loads[1].append(into(1, plane_of[0], j, down_own.at[j], big.at[1, 0, j]))
    flipped = (i, i + 1 - 2 * (i % 2), (i + 2) % 4, 3 - i)

    def item_loads(n):
        src, land, k, _ = items[n]
        weights = 0 if n == 0 else 1
        copies = [into(weights, plane_of[k], i, src, big.at[weights, k, 0])]
        for j in range(1, inner):
            copies.append(
                into(weights, plane_of[k], flipped[j], land.at[j - 1], big.at[weights, k, j])
            )
        return copies

    def land_item(n):
        leg(n, items[n][3][1]).wait_recv()
        leg(n, 3).wait_recv()
        copies = item_loads(n)
        for copy in copies:
            copy.start()
        return copies

    send_item(0)
    send_item(1)
    for copy in loads[0] + loads[1]:
        copy.start()

    @pl.when(mid == 1)
    def _():
        own_across.start()

    def given_pair(q):
        return remote(given_s.at[q], given_r.at[q], give_s.at[q], give_r.at[q], to_core)

    block = 512

    def hide(q, first=False):
        src = normed_ref if first else tok_a.at[q]
        own_in = pltpu.make_async_copy(src, tok_v.at[core], loc.at[0])
        own_in.start()
        token_pair(q).wait_recv()
        other_in = pltpu.make_async_copy(tok_b.at[q], tok_v.at[1 - core], loc.at[1])
        other_in.start()
        own_in.wait()
        other_in.wait()

        @pl.loop(0, units // block)
        def _(n):
            cols = pl.ds(pl.multiple_of(n * block, block), block)
            hidden = jnp.dot(tok_v[0], up_v[:width, cols], preferred_element_type=jnp.float32)
            hidden += jnp.dot(tok_v[1], up_v[width:, cols], preferred_element_type=jnp.float32)
            hidden = jnp.maximum(hidden, 0.0)
            sq_v[q, :, cols] = (hidden * hidden).astype(jnp.bfloat16)

    def keep_rows(q, start, size):
        return pl.ds(pl.multiple_of(q * tok + start, size), size)

    def multiply(q):
        def product(side, put):
            @pl.loop(0, width // block)
            def _(n):
                from_at = pl.multiple_of(side * width + n * block, block)
                part = jnp.dot(
                    sq_v[q], down_v[:, pl.ds(from_at, block)], preferred_element_type=jnp.float32
                )
                put(pl.ds(pl.multiple_of(n * block, block), block), part.astype(jnp.bfloat16))

        def put_stage(cols, part):
            stage_v[:, cols] = part

        def put_keep(cols, part):
            up_v[keep_rows(q, 0, tok), cols] = part

        product(1 - core, put_stage)
        local(stage_v, given_s.at[q], loc.at[2])
        given_pair(q).start()
        product(core, put_keep)

    chunk = 128

    def total(q, start, extra):
        rows = pl.ds(start, chunk)
        value = up_v[keep_rows(q, start, chunk)].astype(jnp.float32)
        value = value + recv_v[rows].astype(jnp.float32)
        if extra:
            value = value + add_v[rows].astype(jnp.float32)
        return value

    def pass_on(q, extra, wait, out, copies):
        given_pair(q).wait_recv()
        one = pltpu.make_async_copy(given_r.at[q], recv_v, loc.at[3])
        one.start()
        one.wait()
        for h in range(2):
            rows = pl.ds(h * half, half)
            if extra is not None:
                wait(h)
                local(extra.at[rows], add_v.at[rows], loc.at[4])

            @pl.loop(0, half // chunk)
            def _(n):
                start = pl.multiple_of(h * half + n * chunk, chunk)
                sum_v[pl.ds(start, chunk)] = total(q, start, extra is not None).astype(jnp.bfloat16)

            local(sum_v.at[rows], out.at[rows], loc.at[5])
            copies(h).start()

    def halves(src, dst, send, recv, peer):
        def copy(h):
            rows = pl.ds(h * half, half)
            return remote(src.at[rows], dst.at[rows], send.at[h], recv.at[h], peer)

        return copy

    to_mid = [
        halves(send_e.at[n], ends_ref.at[n], e_s.at[n], e_r.at[n], to_near) for n in range(3)
    ]
    to_other = [
        halves(send_x.at[n], mids_ref.at[n], x_s.at[n], x_r.at[n], to_across) for n in range(2)
    ]
    to_end = halves(send_l, last_ref, l_s, l_r, to_near)

    forward_item(0)
    forward_item(1)
    send_item(2)
    send_item(3)
    arrived(1)

    @pl.when(mid == 1)
    def _():
        near_across.start()
        arrived(3)
        across_near.start()

    for copy in land_item(0) + loads[0]:
        copy.wait()
    hide(0, True)
    hide(1)
    forward_item(2)
    forward_item(3)
    landed = land_item(1)

    @pl.when(mid == 0)
    def _():
        arrived(2)

    hide(2 + mid)

    @pl.when(mid == 1)
    def _():
        arrived(2)
        far_near.start()

    @pl.when(mid == 0)
    def _():
        arrived(3)

    hide(3 - mid)
    landed = landed + land_item(2) + land_item(3)
    for copy in landed + loads[1]:
        copy.wait()
    multiply(1)

    @pl.when(mid == 0)
    def _():
        pass_on(1, None, None, send_e.at[0], to_mid[0])

    multiply(2 + mid)

    @pl.when(mid == 0)
    def _():
        pass_on(2, None, None, send_e.at[1], to_mid[1])

    multiply(3 - mid)

    @pl.when(mid == 0)
    def _():
        pass_on(3, None, None, send_e.at[2], to_mid[2])

    multiply(0)

    @pl.when(mid == 1)
    def _():
        pass_on(3, ends_ref.at[1], lambda h: to_mid[1](h).wait_recv(), send_x.at[0], to_other[0])
        pass_on(2, ends_ref.at[2], lambda h: to_mid[2](h).wait_recv(), send_x.at[1], to_other[1])
        pass_on(1, mids_ref.at[1], lambda h: to_other[1](h).wait_recv(), send_l, to_end)

    given_pair(0).wait_recv()
    local(given_r.at[0], recv_v, loc.at[3])

    @pl.loop(0, tok // chunk)
    def _(n):
        start = pl.multiple_of(n * chunk, chunk)
        sum_v[pl.ds(start, chunk)] = total(0, start, False).astype(jnp.bfloat16)

    local(sum_v, own_ref, loc.at[5])

    @pl.when(mid == 0)
    def _():
        for h in range(2):
            to_end(h).wait_recv()
            for n in range(3):
                to_mid[n](h).wait_send()

    @pl.when(mid == 1)
    def _():
        own_across.wait_send()
        near_across.wait_send()
        across_near.wait_send()
        far_near.wait_send()
        for h in range(2):
            to_mid[0](h).wait_recv()
            to_other[0](h).wait_recv()
            for n in range(2):
                to_other[n](h).wait_send()
            to_end(h).wait_send()

    own_near.wait_send()
    for n in range(len(items)):
        for j in range(1, inner):
            leg(n, j).wait_send()
    for q in range(outer):
        token_pair(q).wait_send()
        given_pair(q).wait_send()


def feed_forward(normed, up_own, up_odd, down_own, late, inner, outer):
    tok, width = normed.shape
    depth, units = late[0].shape
    block = lambda *lead: jax.ShapeDtypeStruct(lead + (tok, width), jnp.bfloat16)
    any_space = pl.BlockSpec(memory_space=pl.ANY)
    outs = [block(), block(3), block(2), block()]
    outs += [block(outer), block(outer), block(outer), block(outer), block(3), block(2), block()]
    outs += [
        jax.ShapeDtypeStruct((inner - 1, depth, units), jnp.bfloat16),
        jax.ShapeDtypeStruct((3, inner - 1, units, depth), jnp.bfloat16),
    ]
    dma = pltpu.SemaphoreType.DMA
    vmem = lambda *shape: pltpu.VMEM(shape, jnp.bfloat16)
    flops = 8 * outer * tok * width * units
    return pl.pallas_call(
        functools.partial(feed_kernel, outer, inner, tok, width, units),
        out_shape=outs,
        in_specs=[any_space] * (4 + len(late)),
        out_specs=[any_space] * len(outs),
        scratch_shapes=[
            vmem(2 * width, units),
            vmem(units, 2 * width),
            vmem(2, tok, width),
            vmem(outer, tok, units),
            vmem(tok, width),
            vmem(tok, width),
            vmem(tok, width),
            vmem(tok, width),
            dma((5,)), dma((outer,)), dma((outer,)), dma((outer,)), dma((outer,)), dma((outer,)),
            dma((3, 2)), dma((3, 2)), dma((2, 2)), dma((2, 2)), dma((2,)), dma((2,)),
            dma((4, inner - 1)), dma((4, inner - 1)), dma((6,)), dma((2, outer, inner)),
        ],
        compiler_params=pltpu.CompilerParams(
            collective_id=0, has_side_effects=True, vmem_limit_bytes=63 * 1024 * 1024
        ),
        cost_estimate=pl.CostEstimate(flops=flops, bytes_accessed=0, transcendentals=0),
        name="feed_forward",
    )(normed, up_own, up_odd, down_own, *late)[:4]


def split_body(
    inner,
    outer,
    queries,
    keys,
    values,
    documents,
    query_gain,
    key_gain,
    residual,
    out_weight,
    norm_gain,
    up_weight,
    down_weight,
):
    tok = queries.shape[0]
    group = HQ // KV
    width = residual.shape[1]
    units = up_weight.shape[1] // outer
    size = inner * outer
    me = lax.axis_index("sp")
    core = lax.axis_index("tp")
    z = me // inner
    i = me % inner

    def flip(array, bits):
        return lax.ppermute(array, "sp", [(s, s ^ bits) for s in range(size)])

    def partner(array):
        return lax.ppermute(array, "tp", [(0, 1), (1, 0)])

    def line(array, step):
        pairs = [
            (s, s + step * inner) for s in range(size) if 0 <= s // inner + step < outer
        ]
        return lax.ppermute(array, "sp", pairs)

    def gather_line(array):
        right, left = [array], [array]
        for _ in range(1, outer):
            right.append(line(right[-1], 1))
            left.append(line(left[-1], -1))
        return [array] + [
            jnp.where(z >= r, right[r], left[outer - r]) for r in range(1, outer)
        ]

    def after(array, *others):
        return lax.optimization_barrier((array,) + others)[0]

    planes = [[p * inner + j for j in range(inner)] for p in range(outer)]

    def spread(block):
        return lax.all_gather(block, "sp", axis=0, axis_index_groups=planes, tiled=False)

    positions = me * tok + jnp.arange(tok, dtype=jnp.int32)
    packed = prepare(queries, keys, values, positions, query_gain, key_gain)
    cols = 2 * HD
    doc_rows = tok // cols
    notes = jnp.zeros((doc_pad, (group + 2) * HD), jnp.bfloat16)
    notes = notes.at[:doc_rows, group * HD :].set(
        documents.astype(jnp.bfloat16).reshape(doc_rows, cols)
    )
    notes = jnp.broadcast_to(notes[None], (inner,) + notes.shape)
    packed = jnp.concatenate([packed, notes], axis=1)

    def moved(weight, k, axis, *gates):
        block = lax.dynamic_slice_in_dim(weight, (z ^ k) * units, units, axis)
        if gates:
            block = after(block, *gates)
        return flip(block, k * inner)

    early_1 = moved(up_weight, 1, 1)
    early_3 = moved(up_weight, 3, 1)

    mine = jnp.zeros((inner,) + packed.shape[1:], jnp.bfloat16)
    for m in range(inner):
        piece = lax.dynamic_index_in_dim(packed, i ^ m, 0, keepdims=False)
        if m:
            piece = flip(piece, m)
        mine = lax.dynamic_update_index_in_dim(mine, piece, i ^ m, 0)
    key_slots = gather_line(mine[:, :, group * HD :].reshape(-1, cols))
    key_value = jnp.stack(key_slots)

    up_own = spread(after(lax.dynamic_slice_in_dim(up_weight, z * units, units, 1), mine))
    up_odd = spread(jnp.concatenate([after(early_1, key_value), early_3], axis=0))
    down_own = spread(
        after(lax.dynamic_slice_in_dim(down_weight, z * units, units, 0), key_value)
    )
    late_u2 = moved(up_weight, 2, 1, key_value)
    late_d2 = moved(down_weight, 2, 0, key_value)
    late_d3 = moved(down_weight, 3, 0, key_value)
    late_d1 = moved(down_weight, 1, 0, key_value)

    docs = key_value.reshape(outer, inner, tok + doc_pad, cols)[:, :, tok : tok + doc_rows]
    docs = docs.reshape(outer, inner * tok).astype(jnp.int32)
    docs = docs[(z - jnp.arange(outer)) % outer].reshape(-1)
    attended = attention(
        mine[:, :tok].reshape(inner * tok, -1),
        key_value.reshape(outer * inner, tok + doc_pad, cols),
        docs, z, group, outer,
    )
    attended = attended.reshape(inner, tok, group * HD)
    pieces, rows = [], []
    for m in range(inner):
        piece = lax.dynamic_index_in_dim(attended, i ^ m, 0, keepdims=False)
        pieces.append(flip(piece, m) if m else piece)
        rows.append(lax.dynamic_slice_in_dim(out_weight, (i ^ m) * group * HD, group * HD, 0))
    rows = after(jnp.concatenate(rows, axis=0), packed)
    heads = jnp.concatenate(pieces, axis=1)
    partial_out = jnp.dot(heads, rows, preferred_element_type=jnp.float32)
    partial_out = partial_out.astype(jnp.bfloat16)
    kept = lax.dynamic_slice_in_dim(partial_out, core * width, width, 1)
    given = lax.dynamic_slice_in_dim(partial_out, (1 - core) * width, width, 1)
    branch = kept.astype(jnp.float32) + partner(given).astype(jnp.float32)
    stream = residual.astype(jnp.float32) + branch
    squares = jnp.sum(stream * stream, axis=-1, keepdims=True)
    squares = squares + partner(squares)
    gain = lax.dynamic_slice_in_dim(norm_gain, core * width, width)
    normed = stream * lax.rsqrt(squares / (2 * width) + norm_eps) * gain
    normed = normed.astype(jnp.bfloat16)
    late = (late_u2, late_d2, late_d3, late_d1)

    own, ends, mids, last = feed_forward(normed, up_own, up_odd, down_own, late, inner, outer)
    middle = (z > 0) & (z < outer - 1)
    come = jnp.where(
        middle,
        ends[0].astype(jnp.float32) + mids[0].astype(jnp.float32),
        last.astype(jnp.float32),
    )
    return (stream + own.astype(jnp.float32) + come).astype(jnp.bfloat16)


def solution(mesh):
    in_specs = (
        P("sp", "tp"),
        P("sp", "tp"),
        P("sp", "tp"),
        P("sp"),
        P(),
        P(),
        P("sp", "tp"),
        P("tp", None),
        P(),
        P("sp", "tp"),
        P("tp", "sp"),
    )
    out_specs = P("sp", "tp")
    sp, tp = mesh.shape["sp"], mesh.shape["tp"]
    inner = KV // tp
    body = gather_body
    if tp == 2 and inner == 4 and sp % inner == 0 and sp // inner == 4:
        split = functools.partial(split_body, inner, sp // inner)

        def body(*args):
            return split(*args)

    return jax.shard_map(body, mesh=mesh, in_specs=in_specs, out_specs=out_specs, check_vma=False)
```

```python
import functools

import jax
import jax.numpy as jnp
from jax import lax
from jax.experimental import pallas as pl
from jax.experimental.layout import Layout, with_layout_constraint
from jax.experimental.pallas import tpu as pltpu
from jax.sharding import PartitionSpec as P


HQ = 16
KV = 8
HD = 128
GRID_W = 64


norm_eps = 1e-06
rope_base = 10000.0
masked_score = -1e30
log2e = 1.4426950408889634


def head_norm(heads_in, gain):
    values32 = heads_in.astype(jnp.float32)
    scaled = values32 * lax.rsqrt(jnp.mean(values32 * values32, axis=-1, keepdims=True) + norm_eps)
    return scaled * gain


def rotate_half(heads_in, position):
    quarter = heads_in.shape[-1] // 2
    inverse_freq = rope_base ** (-jnp.arange(quarter, dtype=jnp.float32) / quarter)
    angles = position[:, None] * inverse_freq[None, :]
    cosine_part = jnp.cos(angles)[:, None, :]
    sine_part = jnp.sin(angles)[:, None, :]
    leading = heads_in[..., :quarter]
    trailing = heads_in[..., quarter:]
    return jnp.concatenate(
        [
            leading * cosine_part - trailing * sine_part,
            leading * sine_part + trailing * cosine_part,
        ],
        axis=-1,
    )


def grid_rotary(heads_in, positions):
    half_width = heads_in.shape[-1] // 2
    grid_row = (positions // GRID_W).astype(jnp.float32)
    grid_col = (positions % GRID_W).astype(jnp.float32)
    return jnp.concatenate(
        [
            rotate_half(heads_in[..., :half_width], grid_row),
            rotate_half(heads_in[..., half_width:], grid_col),
        ],
        axis=-1,
    )


def row_major(array):
    return with_layout_constraint(array, Layout(major_to_minor=(0, 1)))


def from_behind(array, shift, size):
    return lax.ppermute(array, "tp", [(i, (i + shift) % size) for i in range(size)])


def gather_body(
    queries,
    keys,
    values,
    documents,
    query_gain,
    key_gain,
    residual,
    out_weight,
    norm_gain,
    up_weight,
    down_weight,
):
    tok_rows = queries.shape[0]
    key_heads = keys.shape[1] // HD
    group_size = HQ // KV
    width_local = residual.shape[1]
    tp_index = lax.axis_index("tp")
    up_whole = lax.all_gather(up_weight, "sp", axis=0, tiled=True)
    tp_size = lax.axis_size("tp")
    residual_whole = jnp.zeros((tok_rows, width_local * tp_size), jnp.bfloat16)
    residual_whole = lax.dynamic_update_slice_in_dim(
        residual_whole, residual, tp_index * width_local, 1
    )
    for shift in range(1, tp_size):
        owner = (tp_index - shift) % tp_size
        residual_whole = lax.dynamic_update_slice_in_dim(
            residual_whole, from_behind(residual, shift, tp_size), owner * width_local, 1
        )
    positions = lax.axis_index("sp") * tok_rows + jnp.arange(tok_rows, dtype=jnp.int32)
    queries_rot = grid_rotary(
        head_norm(queries.reshape(tok_rows, key_heads * group_size, HD), query_gain), positions
    )
    queries_rot = queries_rot.astype(jnp.bfloat16).reshape(tok_rows, key_heads, group_size, HD)
    keys_rot = grid_rotary(
        head_norm(keys.reshape(tok_rows, key_heads, HD), key_gain), positions
    ).astype(jnp.bfloat16)
    value_heads = values.reshape(tok_rows, key_heads, HD)
    own_docs = documents.astype(jnp.bfloat16)
    score_scale = HD ** (-0.5)
    key_value = jnp.concatenate(
        [keys_rot.reshape(tok_rows, key_heads * HD), value_heads.reshape(tok_rows, key_heads * HD)],
        axis=1,
    )
    key_value = lax.all_gather(key_value, "sp", axis=0, tiled=True)
    doc_piece = lax.all_gather(own_docs, "sp", axis=0, tiled=True)
    same_doc = own_docs[:, None] == doc_piece[None, :]
    head_queries = queries_rot.reshape(tok_rows, key_heads * group_size, HD).swapaxes(0, 1)

    def attend(query_head):
        head, query = query_head
        key_at = head // group_size * HD
        key_piece = lax.dynamic_slice_in_dim(key_value, key_at, HD, 1)
        value_piece = lax.dynamic_slice_in_dim(key_value, key_at + key_heads * HD, HD, 1)
        scores = jnp.einsum("qd,sd->qs", query, key_piece, preferred_element_type=jnp.float32)
        scores = jnp.where(same_doc, scores * score_scale, masked_score)
        row_max = jnp.max(scores, axis=-1, keepdims=True)
        probs = jnp.where(same_doc, jnp.exp(scores - row_max), 0.0)
        row_sum = jnp.sum(probs, axis=-1)
        update = jnp.dot(
            probs.astype(jnp.bfloat16), value_piece, preferred_element_type=jnp.float32
        )
        return (update / row_sum[:, None]).astype(jnp.bfloat16)

    attended = lax.map(attend, (jnp.arange(key_heads * group_size), head_queries))
    down_late, attended = lax.optimization_barrier((row_major(down_weight.T), attended))
    down_whole = lax.all_gather(down_late, "sp", axis=0, tiled=True)
    attended = attended.swapaxes(0, 1)
    attended = attended.reshape(tok_rows, key_heads * group_size * HD)
    partial_out = jnp.dot(attended, out_weight, preferred_element_type=jnp.float32)
    partial_out = partial_out.astype(jnp.bfloat16)
    branch = partial_out.astype(jnp.float32)
    for shift in range(1, tp_size):
        branch = branch + from_behind(partial_out, shift, tp_size).astype(jnp.float32)
    stream_whole = residual_whole.astype(jnp.float32) + branch
    normed = stream_whole * lax.rsqrt(
        jnp.mean(stream_whole * stream_whole, axis=-1, keepdims=True) + norm_eps
    )
    normed = (normed * norm_gain).astype(jnp.bfloat16)
    stream = lax.dynamic_slice_in_dim(stream_whole, tp_index * width_local, width_local, 1)
    hidden = jnp.dot(normed, up_whole, preferred_element_type=jnp.float32)
    positive = jnp.maximum(hidden, 0.0)
    squared = (positive * positive).astype(jnp.bfloat16)
    product = lax.dot_general(
        squared, down_whole, (((1,), (1,)), ((), ())), preferred_element_type=jnp.float32
    )
    product = product.astype(jnp.bfloat16)
    feed = lax.dynamic_slice_in_dim(product, tp_index * width_local, width_local, 1)
    feed = feed.astype(jnp.float32)
    for shift in range(1, tp_size):
        target = (tp_index + shift) % tp_size
        piece = lax.dynamic_slice_in_dim(product, target * width_local, width_local, 1)
        feed = feed + from_behind(piece, shift, tp_size).astype(jnp.float32)
    return (stream + feed).astype(jnp.bfloat16)


def prepare_kernel(heads, group, q_ref, k_ref, v_ref, cos_ref, sin_ref, qg_ref, kg_ref, o_ref):
    cosine = cos_ref[...]
    sine = sin_ref[...]
    lane = lax.broadcasted_iota(jnp.int32, cosine.shape, 1)
    first = (lane % (HD // 2)) < HD // 4

    def turned(u, gain):
        u = u.astype(jnp.float32)
        u = u * lax.rsqrt(jnp.mean(u * u, axis=-1, keepdims=True) + norm_eps) * gain
        ahead = pltpu.roll(u, HD - HD // 4, 1)
        behind = pltpu.roll(u, HD // 4, 1)
        return (u * cosine + jnp.where(first, ahead, behind) * sine).astype(jnp.bfloat16)

    q_gain = qg_ref[...]
    k_gain = kg_ref[...]
    for h in range(heads):
        for g in range(group):
            at = (h * group + g) * HD
            o_ref[h, :, g * HD : (g + 1) * HD] = turned(q_ref[:, at : at + HD], q_gain)
        at = h * HD
        o_ref[h, :, group * HD : (group + 1) * HD] = turned(k_ref[:, at : at + HD], k_gain)
        o_ref[h, :, (group + 1) * HD :] = v_ref[:, at : at + HD]


def prepare(queries, keys, values, positions, query_gain, key_gain):
    rows = queries.shape[0]
    heads = keys.shape[1] // HD
    group = HQ // KV
    lane = jnp.arange(HD, dtype=jnp.int32)
    quarter = HD // 4
    freq = rope_base ** (-(lane % quarter).astype(jnp.float32) / quarter)
    grid_row = (positions // GRID_W).astype(jnp.float32)
    grid_col = (positions % GRID_W).astype(jnp.float32)
    where_at = jnp.where(lane[None, :] < HD // 2, grid_row[:, None], grid_col[:, None])
    angles = where_at * freq[None, :]
    cosine = jnp.cos(angles)
    sine = jnp.where((lane % (HD // 2)) < quarter, -1.0, 1.0)[None, :] * jnp.sin(angles)
    block = min(rows, 128)
    width = (group + 2) * HD
    row_block = lambda cols: pl.BlockSpec((block, cols), lambda i: (i, 0))
    fixed = pl.BlockSpec((1, HD), lambda i: (0, 0))
    return pl.pallas_call(
        functools.partial(prepare_kernel, heads, group),
        grid=(rows // block,),
        out_shape=jax.ShapeDtypeStruct((heads, rows, width), jnp.bfloat16),
        in_specs=[
            row_block(heads * group * HD),
            row_block(heads * HD),
            row_block(heads * HD),
            row_block(HD),
            row_block(HD),
            fixed,
            fixed,
        ],
        out_specs=pl.BlockSpec((heads, block, width), lambda i: (0, i, 0)),
        cost_estimate=pl.CostEstimate(flops=rows * 20000, bytes_accessed=rows * 8192, transcendentals=0),
        name="prepare",
    )(queries, keys, values, cosine, sine, query_gain.reshape(1, HD), key_gain.reshape(1, HD))


def attend_kernel(group, key_block, slots, span_ref, q_ref, kv_ref, qdoc_ref, kdoc_ref, o_ref):
    tile = pl.program_id(0)
    lo = span_ref[0, tile]
    hi = span_ref[1, tile]
    plane = span_ref[4, tile]
    rows = q_ref.shape[0]
    per_slot = kv_ref.shape[0] // slots
    query = jnp.concatenate([q_ref[:, g * HD : (g + 1) * HD] for g in range(group)], axis=0)
    q_doc = jnp.concatenate([qdoc_ref[...]] * group, axis=0)
    factor = HD ** (-0.5) * log2e

    def step(block, carry):
        top, total, out = carry
        slot = lax.rem(plane + slots - block // per_slot, slots)
        at = slot * per_slot + lax.rem(block, per_slot)
        key = kv_ref[at, :key_block, :HD]
        value = kv_ref[at, :key_block, HD:]
        scores = lax.dot_general(
            query, key, (((1,), (1,)), ((), ())), preferred_element_type=jnp.float32
        )
        k_doc = kdoc_ref[block]
        scores = jnp.where(q_doc == k_doc, scores, masked_score)
        new_top = jnp.maximum(top, jnp.max(scores, axis=-1, keepdims=True))
        probs = jnp.exp2((scores - new_top) * factor)
        fade = jnp.exp2((top - new_top) * factor)
        total = total * fade + jnp.sum(probs, axis=-1, keepdims=True)
        out = out * fade + jnp.dot(
            probs.astype(jnp.bfloat16), value, preferred_element_type=jnp.float32
        )
        return new_top, total, out

    start = (
        jnp.full((group * rows, 1), masked_score, jnp.float32),
        jnp.zeros((group * rows, 1), jnp.float32),
        jnp.zeros((group * rows, HD), jnp.float32),
    )
    _, total, out = lax.fori_loop(lo, hi, step, start)
    out = (out / total).astype(jnp.bfloat16)
    for g in range(group):
        o_ref[:, g * HD : (g + 1) * HD] = out[g * rows : (g + 1) * rows]


doc_pad = 16


def attention(packed, key_value, docs, plane, group, slots):
    rows = packed.shape[0]
    tile = min(256, rows)
    key_block = key_value.shape[1] - doc_pad
    own = lax.dynamic_slice_in_dim(docs, plane * rows, rows)
    q_low = own[::tile]
    q_high = own[tile - 1 :: tile]
    k_low = docs[::key_block]
    k_high = docs[key_block - 1 :: key_block]
    lo = jnp.sum(k_high[None, :] < q_low[:, None], axis=1).astype(jnp.int32)
    hi = jnp.sum(k_low[None, :] <= q_high[:, None], axis=1).astype(jnp.int32)
    span = jnp.stack([lo, hi, q_low, q_high, jnp.full_like(lo, plane)])
    blocks = docs.shape[0] // key_block
    grid_spec = pltpu.PrefetchScalarGridSpec(
        num_scalar_prefetch=1,
        grid=(rows // tile,),
        in_specs=[
            pl.BlockSpec((tile, group * HD), lambda i, s: (i, 0)),
            pl.BlockSpec(key_value.shape, lambda i, s: (0, 0, 0)),
            pl.BlockSpec((tile, 1), lambda i, s: (i, 0)),
            pl.BlockSpec((blocks, 1, key_block), lambda i, s: (0, 0, 0)),
        ],
        out_specs=pl.BlockSpec((tile, group * HD), lambda i, s: (i, 0)),
    )
    work = group * rows * docs.shape[0] // 2
    return pl.pallas_call(
        functools.partial(attend_kernel, group, key_block, slots),
        grid_spec=grid_spec,
        out_shape=jax.ShapeDtypeStruct((rows, group * HD), jnp.bfloat16),
        compiler_params=pltpu.CompilerParams(vmem_limit_bytes=48 * 1024 * 1024),
        cost_estimate=pl.CostEstimate(
            flops=work * 4 * HD, bytes_accessed=key_value.size * 2, transcendentals=work
        ),
        name="attention",
    )(span, packed, key_value, own.reshape(rows, 1), docs.reshape(blocks, 1, key_block))


MESH = pl.DeviceIdType.MESH


def feed_kernel(
    outer, inner, tok, width, units,
    normed_ref, up_own, up_odd, down_own, late_u2, late_d2, late_d3, late_d1,
    own_ref, ends_ref, mids_ref, last_ref, tok_a, tok_b, given_s, given_r, send_e, send_x, send_l, land_u, land_d,
    up_v, down_v, tok_v, sq_v, stage_v, recv_v, recv_w, add_v, sum_v,
    way_s, way_r, pair_s, pair_r, give_s, give_r, e_s, e_r, x_s, x_r, l_s, l_r, w_s, w_r, loc, big,
):
    me = lax.axis_index("sp")
    core = lax.axis_index("tp")
    z = me // inner
    i = me % inner
    mid = ((z + 1) // 2) % 2
    near = (z + 1 - 2 * (z % 2)) * inner + i
    across = (outer - 1 - z) * inner + i
    parts = 4
    half = tok // parts

    barrier = pltpu.get_barrier_semaphore()
    beside = [{"sp": z * inner + i + bit - 2 * bit * ((i // bit) % 2)} for bit in (1, 2)]
    for peer in ({"sp": near}, {"sp": across}, {"tp": 1 - core}, *beside):
        pl.semaphore_signal(barrier, inc=1, device_id=peer, device_id_type=MESH)
    pl.semaphore_wait(barrier, 5)

    def remote(src, dst, send, recv, peer):
        return pltpu.make_async_remote_copy(
            src_ref=src, dst_ref=dst, send_sem=send, recv_sem=recv, device_id=peer, device_id_type=MESH
        )

    def local(src, dst, sem):
        copy = pltpu.make_async_copy(src, dst, sem)
        copy.start()
        copy.wait()

    to_near, to_across, to_core = {"sp": near}, {"sp": across}, {"tp": 1 - core}
    own_near = remote(normed_ref, tok_a.at[1], way_s.at[0], way_r.at[1], to_near)
    own_across = remote(normed_ref, tok_a.at[3], way_s.at[1], way_r.at[3], to_across)
    near_across = remote(tok_a.at[1], tok_a.at[2], way_s.at[2], way_r.at[2], to_across)
    across_near = remote(tok_a.at[3], tok_a.at[2], way_s.at[3], way_r.at[2], to_near)
    far_near = remote(tok_a.at[2], tok_a.at[3], way_s.at[4], way_r.at[3], to_near)

    def token_pair(q):
        src = normed_ref if isinstance(q, int) and q == 0 else tok_a.at[q]
        return remote(src, tok_b.at[q], pair_s.at[q], pair_r.at[q], to_core)

    def arrived(q):
        remote(tok_a.at[q], tok_a.at[q], way_s.at[0], way_r.at[q], to_near).wait_recv()
        token_pair(q).start()

    own_near.start()
    token_pair(0).start()
    depth = late_u2.shape[0]
    plane_of = (z, z + 1 - 2 * (z % 2), (z + 2) % 4, 3 - z)
    peers = {bit: {"sp": z * inner + i + bit - 2 * bit * ((i // bit) % 2)} for bit in (1, 2)}
    items = [
        (late_u2, land_u, 2, (1, 2)),
        (late_d2, land_d.at[0], 2, (2, 1)),
        (late_d3, land_d.at[1], 3, (1, 2)),
        (late_d1, land_d.at[2], 1, (2, 1)),
    ]

    def leg(n, j):
        src, land, _, (first, second) = items[n]
        from_ref = src if j < 3 else land.at[first - 1]
        return remote(
            from_ref, land.at[j - 1], w_s.at[n, j - 1], w_r.at[n, j - 1], peers[second if j == 3 else j]
        )

    def send_item(n):
        first, second = items[n][3]
        leg(n, first).start()
        leg(n, second).start()

    def forward_item(n):
        leg(n, items[n][3][0]).wait_recv()
        leg(n, 3).start()

    def into(weights, plane, j, src, sem):
        at = pl.ds(pl.multiple_of((plane * inner + j) * depth, depth), depth)
        dst = up_v.at[at] if weights == 0 else down_v.at[:, at]
        return pltpu.make_async_copy(src, dst, sem)

    loads = [], []
    for j in range(inner):
        loads[0].append(into(0, plane_of[0], j, up_own.at[j], big.at[0, 0, j]))
        for n, k in enumerate((1, 3)):
            src = up_odd.at[j, n * depth : (n + 1) * depth]
            loads[0].append(into(0, plane_of[k], j, src, big.at[0, k, j]))
        loads[1].append(into(1, plane_of[0], j, down_own.at[j], big.at[1, 0, j]))
    flipped = (i, i + 1 - 2 * (i % 2), (i + 2) % 4, 3 - i)

    def item_loads(n):
        src, land, k, _ = items[n]
        weights = 0 if n == 0 else 1
        copies = [into(weights, plane_of[k], i, src, big.at[weights, k, 0])]
        for j in range(1, inner):
            copies.append(
                into(weights, plane_of[k], flipped[j], land.at[j - 1], big.at[weights, k, j])
            )
        return copies

    def land_item(n):
        leg(n, items[n][3][1]).wait_recv()
        leg(n, 3).wait_recv()
        copies = item_loads(n)
        for copy in copies:
            copy.start()
        return copies

    send_item(0)
    send_item(1)
    for copy in loads[0] + loads[1]:
        copy.start()

    @pl.when(mid == 1)
    def _():
        own_across.start()

    def given_pair(q):
        return remote(given_s.at[q], given_r.at[q], give_s.at[q], give_r.at[q], to_core)

    block = 512

    def hide(q, first=False):
        src = normed_ref if first else tok_a.at[q]
        own_in = pltpu.make_async_copy(src, tok_v.at[core], loc.at[0])
        own_in.start()
        token_pair(q).wait_recv()
        other_in = pltpu.make_async_copy(tok_b.at[q], tok_v.at[1 - core], loc.at[1])
        other_in.start()
        own_in.wait()
        other_in.wait()

        @pl.loop(0, units // block)
        def _(n):
            cols = pl.ds(pl.multiple_of(n * block, block), block)
            hidden = jnp.dot(tok_v[0], up_v[:width, cols], preferred_element_type=jnp.float32)
            hidden += jnp.dot(tok_v[1], up_v[width:, cols], preferred_element_type=jnp.float32)
            hidden = jnp.maximum(hidden, 0.0)
            sq_v[q, :, cols] = (hidden * hidden).astype(jnp.bfloat16)

    def keep_rows(q, start, size):
        return pl.ds(pl.multiple_of(q * tok + start, size), size)

    def multiply(q):
        def product(side, put):
            @pl.loop(0, width // block)
            def _(n):
                from_at = pl.multiple_of(side * width + n * block, block)
                part = jnp.dot(
                    sq_v[q], down_v[:, pl.ds(from_at, block)], preferred_element_type=jnp.float32
                )
                put(pl.ds(pl.multiple_of(n * block, block), block), part.astype(jnp.bfloat16))

        def put_stage(cols, part):
            stage_v[:, cols] = part

        def put_keep(cols, part):
            up_v[keep_rows(q, 0, tok), cols] = part

        product(1 - core, put_stage)
        local(stage_v, given_s.at[q], loc.at[2])
        given_pair(q).start()
        product(core, put_keep)

    chunk = 128

    def total(q, share, start, extra):
        rows = pl.ds(start, chunk)
        value = up_v[keep_rows(q, start, chunk)].astype(jnp.float32)
        value = value + share[rows].astype(jnp.float32)
        if extra:
            value = value + add_v[rows].astype(jnp.float32)
        return value

    def load_share(q, share):
        given_pair(q).wait_recv()
        local(given_r.at[q], share, loc.at[3])

    def piece_on(h, q, share, extra, wait, out, copies):
        rows = pl.ds(h * half, half)
        if extra is not None:
            wait(h)
            local(extra.at[rows], add_v.at[rows], loc.at[4])

        @pl.loop(0, half // chunk)
        def _(n):
            start = pl.multiple_of(h * half + n * chunk, chunk)
            sum_v[pl.ds(start, chunk)] = total(q, share, start, extra is not None).astype(jnp.bfloat16)

        local(sum_v.at[rows], out.at[rows], loc.at[5])
        copies(h).start()

    def pass_on(q, extra, wait, out, copies):
        load_share(q, recv_v)
        for h in range(parts):
            piece_on(h, q, recv_v, extra, wait, out, copies)

    def halves(src, dst, send, recv, peer):
        def copy(h):
            rows = pl.ds(h * half, half)
            return remote(src.at[rows], dst.at[rows], send.at[h], recv.at[h], peer)

        return copy

    to_mid = [
        halves(send_e.at[n], ends_ref.at[n], e_s.at[n], e_r.at[n], to_near) for n in range(3)
    ]
    to_other = [
        halves(send_x.at[n], mids_ref.at[n], x_s.at[n], x_r.at[n], to_across) for n in range(2)
    ]
    to_end = halves(send_l, last_ref, l_s, l_r, to_near)

    forward_item(0)
    forward_item(1)
    send_item(2)
    send_item(3)
    arrived(1)

    @pl.when(mid == 1)
    def _():
        near_across.start()
        arrived(3)
        across_near.start()

    for copy in land_item(0) + loads[0]:
        copy.wait()
    hide(0, True)
    hide(1)
    arrived(2)

    @pl.when(mid == 1)
    def _():
        far_near.start()

    forward_item(2)
    landed = land_item(1)
    forward_item(3)
    hide(2 + mid)

    @pl.when(mid == 0)
    def _():
        arrived(3)

    hide(3 - mid)
    landed = landed + land_item(2) + land_item(3)
    for copy in landed + loads[1]:
        copy.wait()
    multiply(1)

    @pl.when(mid == 0)
    def _():
        pass_on(1, None, None, send_e.at[0], to_mid[0])

    multiply(2 + mid)

    @pl.when(mid == 0)
    def _():
        pass_on(2, None, None, send_e.at[1], to_mid[1])

    multiply(3 - mid)

    @pl.when(mid == 0)
    def _():
        pass_on(3, None, None, send_e.at[2], to_mid[2])

    multiply(0)

    @pl.when(mid == 1)
    def _():
        pass_on(3, ends_ref.at[1], lambda h: to_mid[1](h).wait_recv(), send_x.at[0], to_other[0])
        load_share(2, recv_v)
        load_share(1, recv_w)
        onward = (2, recv_v, ends_ref.at[2], lambda h: to_mid[2](h).wait_recv(), send_x.at[1], to_other[1])
        home = (1, recv_w, mids_ref.at[1], lambda h: to_other[1](h).wait_recv(), send_l, to_end)
        for h in range(parts):
            piece_on(h, *onward)
            if h:
                piece_on(h - 1, *home)
        piece_on(parts - 1, *home)

    given_pair(0).wait_recv()
    local(given_r.at[0], recv_v, loc.at[3])

    @pl.loop(0, tok // chunk)
    def _(n):
        start = pl.multiple_of(n * chunk, chunk)
        sum_v[pl.ds(start, chunk)] = total(0, recv_v, start, False).astype(jnp.bfloat16)

    local(sum_v, own_ref, loc.at[5])

    @pl.when(mid == 0)
    def _():
        for h in range(parts):
            to_end(h).wait_recv()
            for n in range(3):
                to_mid[n](h).wait_send()

    @pl.when(mid == 1)
    def _():
        own_across.wait_send()
        near_across.wait_send()
        across_near.wait_send()
        far_near.wait_send()
        for h in range(parts):
            to_mid[0](h).wait_recv()
            to_other[0](h).wait_recv()
            for n in range(2):
                to_other[n](h).wait_send()
            to_end(h).wait_send()

    own_near.wait_send()
    for n in range(len(items)):
        for j in range(1, inner):
            leg(n, j).wait_send()
    for q in range(outer):
        token_pair(q).wait_send()
        given_pair(q).wait_send()


def feed_forward(normed, up_own, up_odd, down_own, late, inner, outer):
    tok, width = normed.shape
    depth, units = late[0].shape
    block = lambda *lead: jax.ShapeDtypeStruct(lead + (tok, width), jnp.bfloat16)
    any_space = pl.BlockSpec(memory_space=pl.ANY)
    outs = [block(), block(3), block(2), block()]
    outs += [block(outer), block(outer), block(outer), block(outer), block(3), block(2), block()]
    outs += [
        jax.ShapeDtypeStruct((inner - 1, depth, units), jnp.bfloat16),
        jax.ShapeDtypeStruct((3, inner - 1, units, depth), jnp.bfloat16),
    ]
    dma = pltpu.SemaphoreType.DMA
    vmem = lambda *shape: pltpu.VMEM(shape, jnp.bfloat16)
    flops = 8 * outer * tok * width * units
    return pl.pallas_call(
        functools.partial(feed_kernel, outer, inner, tok, width, units),
        out_shape=outs,
        in_specs=[any_space] * (4 + len(late)),
        out_specs=[any_space] * len(outs),
        scratch_shapes=[
            vmem(2 * width, units),
            vmem(units, 2 * width),
            vmem(2, tok, width),
            vmem(outer, tok, units),
            vmem(tok, width),
            vmem(tok, width),
            vmem(tok, width),
            vmem(tok, width),
            vmem(tok, width),
            dma((5,)), dma((outer,)), dma((outer,)), dma((outer,)), dma((outer,)), dma((outer,)),
            dma((3, 4)), dma((3, 4)), dma((2, 4)), dma((2, 4)), dma((4,)), dma((4,)),
            dma((4, inner - 1)), dma((4, inner - 1)), dma((6,)), dma((2, outer, inner)),
        ],
        compiler_params=pltpu.CompilerParams(
            collective_id=0, has_side_effects=True, vmem_limit_bytes=63 * 1024 * 1024
        ),
        cost_estimate=pl.CostEstimate(flops=flops, bytes_accessed=0, transcendentals=0),
        name="feed_forward",
    )(normed, up_own, up_odd, down_own, *late)[:4]


def split_body(
    inner,
    outer,
    queries,
    keys,
    values,
    documents,
    query_gain,
    key_gain,
    residual,
    out_weight,
    norm_gain,
    up_weight,
    down_weight,
):
    tok = queries.shape[0]
    group = HQ // KV
    width = residual.shape[1]
    units = up_weight.shape[1] // outer
    size = inner * outer
    me = lax.axis_index("sp")
    core = lax.axis_index("tp")
    z = me // inner
    i = me % inner

    def flip(array, bits):
        return lax.ppermute(array, "sp", [(s, s ^ bits) for s in range(size)])

    def partner(array):
        return lax.ppermute(array, "tp", [(0, 1), (1, 0)])

    def line(array, step):
        pairs = [
            (s, s + step * inner) for s in range(size) if 0 <= s // inner + step < outer
        ]
        return lax.ppermute(array, "sp", pairs)

    def gather_line(array):
        right, left = [array], [array]
        for _ in range(1, outer):
            right.append(line(right[-1], 1))
            left.append(line(left[-1], -1))
        return [array] + [
            jnp.where(z >= r, right[r], left[outer - r]) for r in range(1, outer)
        ]

    def after(array, *others):
        return lax.optimization_barrier((array,) + others)[0]

    planes = [[p * inner + j for j in range(inner)] for p in range(outer)]

    def spread(block):
        return lax.all_gather(block, "sp", axis=0, axis_index_groups=planes, tiled=False)

    positions = me * tok + jnp.arange(tok, dtype=jnp.int32)
    packed = prepare(queries, keys, values, positions, query_gain, key_gain)
    cols = 2 * HD
    doc_rows = tok // cols
    notes = jnp.zeros((doc_pad, (group + 2) * HD), jnp.bfloat16)
    notes = notes.at[:doc_rows, group * HD :].set(
        documents.astype(jnp.bfloat16).reshape(doc_rows, cols)
    )
    notes = jnp.broadcast_to(notes[None], (inner,) + notes.shape)
    packed = jnp.concatenate([packed, notes], axis=1)

    def moved(weight, k, axis, *gates):
        block = lax.dynamic_slice_in_dim(weight, (z ^ k) * units, units, axis)
        if gates:
            block = after(block, *gates)
        return flip(block, k * inner)

    early_1 = moved(up_weight, 1, 1)
    early_3 = moved(up_weight, 3, 1)

    mine = jnp.zeros((inner,) + packed.shape[1:], jnp.bfloat16)
    for m in range(inner):
        piece = lax.dynamic_index_in_dim(packed, i ^ m, 0, keepdims=False)
        if m:
            piece = flip(piece, m)
        mine = lax.dynamic_update_index_in_dim(mine, piece, i ^ m, 0)
    key_slots = gather_line(mine[:, :, group * HD :].reshape(-1, cols))
    key_value = jnp.stack(key_slots)

    up_own = spread(after(lax.dynamic_slice_in_dim(up_weight, z * units, units, 1), mine))
    up_odd = spread(jnp.concatenate([after(early_1, key_value), early_3], axis=0))
    down_own = spread(
        after(lax.dynamic_slice_in_dim(down_weight, z * units, units, 0), key_value)
    )
    late_u2 = moved(up_weight, 2, 1, key_value)
    late_d2 = moved(down_weight, 2, 0, key_value)
    late_d3 = moved(down_weight, 3, 0, key_value)
    late_d1 = moved(down_weight, 1, 0, key_value)

    docs = key_value.reshape(outer, inner, tok + doc_pad, cols)[:, :, tok : tok + doc_rows]
    docs = docs.reshape(outer, inner * tok).astype(jnp.int32)
    docs = docs[(z - jnp.arange(outer)) % outer].reshape(-1)
    attended = attention(
        mine[:, :tok].reshape(inner * tok, -1),
        key_value.reshape(outer * inner, tok + doc_pad, cols),
        docs, z, group, outer,
    )
    attended = attended.reshape(inner, tok, group * HD)
    pieces, rows = [], []
    for m in range(inner):
        piece = lax.dynamic_index_in_dim(attended, i ^ m, 0, keepdims=False)
        pieces.append(flip(piece, m) if m else piece)
        rows.append(lax.dynamic_slice_in_dim(out_weight, (i ^ m) * group * HD, group * HD, 0))
    rows = after(jnp.concatenate(rows, axis=0), packed)
    heads = jnp.concatenate(pieces, axis=1)
    partial_out = jnp.dot(heads, rows, preferred_element_type=jnp.float32)
    partial_out = partial_out.astype(jnp.bfloat16)
    kept = lax.dynamic_slice_in_dim(partial_out, core * width, width, 1)
    given = lax.dynamic_slice_in_dim(partial_out, (1 - core) * width, width, 1)
    branch = kept.astype(jnp.float32) + partner(given).astype(jnp.float32)
    stream = residual.astype(jnp.float32) + branch
    squares = jnp.sum(stream * stream, axis=-1, keepdims=True)
    squares = squares + partner(squares)
    gain = lax.dynamic_slice_in_dim(norm_gain, core * width, width)
    normed = stream * lax.rsqrt(squares / (2 * width) + norm_eps) * gain
    normed = normed.astype(jnp.bfloat16)
    late = (late_u2, late_d2, late_d3, late_d1)

    own, ends, mids, last = feed_forward(normed, up_own, up_odd, down_own, late, inner, outer)
    middle = (z > 0) & (z < outer - 1)
    come = jnp.where(
        middle,
        ends[0].astype(jnp.float32) + mids[0].astype(jnp.float32),
        last.astype(jnp.float32),
    )
    return (stream + own.astype(jnp.float32) + come).astype(jnp.bfloat16)


def solution(mesh):
    in_specs = (
        P("sp", "tp"),
        P("sp", "tp"),
        P("sp", "tp"),
        P("sp"),
        P(),
        P(),
        P("sp", "tp"),
        P("tp", None),
        P(),
        P("sp", "tp"),
        P("tp", "sp"),
    )
    out_specs = P("sp", "tp")
    sp, tp = mesh.shape["sp"], mesh.shape["tp"]
    inner = KV // tp
    body = gather_body
    if tp == 2 and inner == 4 and sp % inner == 0 and sp // inner == 4:
        split = functools.partial(split_body, inner, sp // inner)

        def body(*args):
            return split(*args)

    return jax.shard_map(body, mesh=mesh, in_specs=in_specs, out_specs=out_specs, check_vma=False)
```
